32 devices in a mesh: sp: 8 (over z, y), tp: 4 (over x, core).
Axes of the slice: x: 2, y: 2, z: 4, core: 2. Of those that a mesh axis runs over, the one named last changes fastest.
Arguments:
- stream: bfloat16 [4096, 2048], P(('sp', 'tp')), may hold values from -6 to 6
- conv_in_a: bfloat16 [4096, 1024], P('sp', 'tp'), may hold values from -6 to 6
- conv_in_b: bfloat16 [4096, 1024], P('sp', 'tp'), may hold values from -6 to 6
- gate_in_a: bfloat16 [4096, 1024], P('sp', 'tp'), may hold values from -6 to 6
- gate_in_b: bfloat16 [4096, 1024], P('sp', 'tp'), may hold values from -6 to 6
- conv_w_a: bfloat16 [4, 1024], P(None, 'tp'), may hold values from -3 to 3
- conv_w_b: bfloat16 [4, 1024], P(None, 'tp'), may hold values from -3 to 3
- rec_gate_a: bfloat16 [16, 64, 64], P('tp'), may hold values from -0.75 to 0.75
- inp_gate_a: bfloat16 [16, 64, 64], P('tp'), may hold values from -0.75 to 0.75
- rec_gate_b: bfloat16 [8, 128, 128], P('tp'), may hold values from -0.5 to 0.5
- inp_gate_b: bfloat16 [8, 128, 128], P('tp'), may hold values from -0.5 to 0.5
- decay_a: float32 [1024], P('tp'), may hold values from 3 to 20
- decay_b: float32 [1024], P('tp'), may hold values from 3 to 20
- decay_increments: float32 [4096], P('sp'), may hold values from -0.7 to 0
- out_w_a: bfloat16 [1024, 2048], P('tp'), may hold values from -0.5 to 0.5
- out_w_b: bfloat16 [1024, 2048], P('tp'), may hold values from -0.5 to 0.5
- norm_gain: bfloat16 [2048], replicated, may hold values from 0.099609375 to 1.8984375
- expert_ids: int32 [4096, 2], P(('sp', 'tp')), may hold values from 0 to 31, as said below
- group_prob: float32 [4096], P(('sp', 'tp')), may hold values from 0.3 to 1
- pick_gap: float32 [4096], P(('sp', 'tp')), may hold values from -6 to 6
- w_gate: bfloat16 [32, 2048, 1024], P(('sp', 'tp')), may hold values from -0.125 to 0.125
- w_up: bfloat16 [32, 2048, 1024], P(('sp', 'tp')), may hold values from -0.125 to 0.125
- w_down: bfloat16 [32, 1024, 2048], P(('sp', 'tp')), may hold values from -0.5 to 0.5
Outputs:
- result: bfloat16 [4096, 2048], P(('sp', 'tp'))
The draws below stay inside these ranges and needn't reach their ends.
Inputs may be any that keep to these rules, and one draw needn't show every extreme that they name: `expert_ids`: each row names two different experts of one group: both lie in g * 8 to g * 8 + 7 for some g. In each aligned block of 128 rows no expert is named more than 16 times, and in every block some expert is named exactly 16 times.
All inputs are finite; a program needn't handle non-finite values.
Results may differ from the reference program's by a relative error of at most 0.015.
Values may be sent and summed in bfloat16 or wider, within the bound.
A program may use at most 128 MiB of HBM per device.

```python
import math
import jax
import jax.numpy as jnp
from jax import lax

D = 2048
HEADS_A = 16
DIM_A = 64
HEADS_B = 8
DIM_B = 128
WIDTH_A = 1024
WIDTH_B = 1024
D_LRU = 2048
CONV_TAPS = 4
FFN_HIDDEN = 1024
EXPERTS = 32
GROUPS = 4
SEQUENCE_TOKENS = 4096
ROWS = 128
CAP = 16


def decay_levels(base_key, head_count, head_dim):
    random_subkeys = jax.random.split(base_key, 4)
    slow_share = 0.5
    is_slow = jax.random.uniform(random_subkeys[0], (head_count,), jnp.float32) < slow_share
    slow_rate = jnp.exp(jax.random.uniform(random_subkeys[1], (head_count,), jnp.float32, math.log(0.05 / SEQUENCE_TOKENS), math.log(0.5 / SEQUENCE_TOKENS)))
    fast_rate = jnp.exp(jax.random.uniform(random_subkeys[2], (head_count,), jnp.float32, math.log(0.004), math.log(0.03)))
    head_rate = jnp.where(is_slow, slow_rate, fast_rate)
    spread = jnp.exp(jax.random.uniform(random_subkeys[3], (head_count * head_dim,), jnp.float32, -0.35, 0.35))
    channel_rate = jnp.repeat(head_rate, head_dim) * spread
    return (-jnp.log(jnp.expm1(channel_rate))).astype(jnp.float32)


def draw_decay_a(key, part):
    return decay_levels(jax.random.fold_in(key, 11), HEADS_A, DIM_A)


def draw_decay_b(key, part):
    return decay_levels(jax.random.fold_in(key, 12), HEADS_B, DIM_B)


def draw_decay_increments(key, part):
    random_subkeys = jax.random.split(jax.random.fold_in(key, 13), 2)
    surge_count = 8
    surge_position = jax.random.randint(random_subkeys[0], (surge_count,), 0, SEQUENCE_TOKENS)
    surge_depth = jnp.log(jax.random.uniform(random_subkeys[1], (surge_count,), jnp.float32, 0.5, 0.8))
    return jnp.zeros((SEQUENCE_TOKENS,), jnp.float32).at[surge_position].set(surge_depth)


def group_order(block_key):
    return jax.random.permutation(block_key, GROUPS)


def row_order(block_key):
    return jax.random.permutation(block_key, ROWS)


def draw_expert_ids(key, part):
    random_subkeys = jax.random.split(jax.random.fold_in(key, 14), 4)
    block_total = SEQUENCE_TOKENS // ROWS
    group_width = EXPERTS // GROUPS
    orders = jax.vmap(group_order)(jax.random.split(random_subkeys[0], block_total))
    offsets = jax.random.randint(random_subkeys[1], (block_total, 3), 0, group_width)
    partner_steps = jax.random.randint(random_subkeys[3], (block_total, 3), 1, group_width)
    position = jnp.arange(ROWS, dtype=jnp.int32)
    half_rows = ROWS // 2
    quarter_rows = ROWS // 4
    slot_rank = (position >= half_rows).astype(jnp.int32) + (position >= half_rows + quarter_rows).astype(jnp.int32)
    starts = jnp.where(slot_rank == 0, 0, jnp.where(slot_rank == 1, half_rows, half_rows + quarter_rows))
    within = position - starts
    rank_rows = jnp.broadcast_to(slot_rank[None, :], (block_total, ROWS))
    group_ids = jnp.take_along_axis(orders, rank_rows, axis=1)
    offset_rows = jnp.take_along_axis(offsets, rank_rows, axis=1)
    step_rows = jnp.take_along_axis(partner_steps, rank_rows, axis=1)
    first_pick = (offset_rows + within[None, :]) % group_width
    second_pick = (first_pick + step_rows) % group_width
    pairs = jnp.stack([group_ids * group_width + first_pick, group_ids * group_width + second_pick], axis=-1)
    shuffles = jax.vmap(row_order)(jax.random.split(random_subkeys[2], block_total))
    pairs = jnp.take_along_axis(pairs, shuffles[:, :, None], axis=1)
    return pairs.reshape(SEQUENCE_TOKENS, 2).astype(jnp.int32)


def block_scale(key, shape, pieces, smallest, largest):
    factor_of = 1.0
    for dim, parts in pieces:
        draws = jax.random.uniform(jax.random.fold_in(jax.random.fold_in(key, 6), dim), (parts,), jnp.float32, smallest / len(pieces), largest / len(pieces))
        factor_of = factor_of * jnp.repeat(jnp.exp(draws), shape[dim] // parts).reshape((-1,) + (1,) * (len(shape) - 1 - dim))
    return factor_of


def noise(key, dims, scale, most, cuts=(), kind=jnp.bfloat16):
    drawn = scale * jax.random.normal(key, dims, jnp.float32)
    if cuts:
        drawn = drawn * block_scale(key, dims, cuts, -0.22, 0.18)
    return jnp.clip(drawn, -most, most).astype(kind)


def setup_inputs(seed: int = 0) -> dict:
    key_of = jax.random.split(jax.random.key(seed), 24)
    return {
        "stream": noise(key_of[0], (SEQUENCE_TOKENS, D), 1.0, 6.0, ((0, 32),)),
        "conv_in_a": noise(key_of[1], (SEQUENCE_TOKENS, WIDTH_A), 1.0, 6.0, ((0, 8), (1, 4))),
        "conv_in_b": noise(key_of[2], (SEQUENCE_TOKENS, WIDTH_B), 1.0, 6.0, ((0, 8), (1, 4))),
        "gate_in_a": noise(key_of[3], (SEQUENCE_TOKENS, WIDTH_A), 1.0, 6.0, ((0, 8), (1, 4))),
        "gate_in_b": noise(key_of[4], (SEQUENCE_TOKENS, WIDTH_B), 1.0, 6.0, ((0, 8), (1, 4))),
        "conv_w_a": noise(key_of[5], (CONV_TAPS, WIDTH_A), CONV_TAPS ** -0.5, 3.0, ((1, 4),)),
        "conv_w_b": noise(key_of[6], (CONV_TAPS, WIDTH_B), CONV_TAPS ** -0.5, 3.0, ((1, 4),)),
        "rec_gate_a": noise(key_of[7], (HEADS_A, DIM_A, DIM_A), DIM_A ** -0.5, 0.75, ((0, 4),)),
        "inp_gate_a": noise(key_of[8], (HEADS_A, DIM_A, DIM_A), DIM_A ** -0.5, 0.75, ((0, 4),)),
        "rec_gate_b": noise(key_of[9], (HEADS_B, DIM_B, DIM_B), DIM_B ** -0.5, 0.5, ((0, 4),)),
        "inp_gate_b": noise(key_of[10], (HEADS_B, DIM_B, DIM_B), DIM_B ** -0.5, 0.5, ((0, 4),)),
        "decay_a": draw_decay_a(jax.random.fold_in(key_of[23], 71), 0),
        "decay_b": draw_decay_b(jax.random.fold_in(key_of[23], 71), 0),
        "decay_increments": draw_decay_increments(jax.random.fold_in(key_of[23], 71), 0),
        "out_w_a": noise(key_of[14], (WIDTH_A, D), (D_LRU // 16) ** -0.5, 0.5, ((0, 4),)),
        "out_w_b": noise(key_of[15], (WIDTH_B, D), (D_LRU // 16) ** -0.5, 0.5, ((0, 4),)),
        "norm_gain": jnp.clip(1.0 + 0.18 * jax.random.normal(key_of[16], (D,), jnp.float32), 0.099609375, 1.8984375).astype(jnp.bfloat16),
        "expert_ids": draw_expert_ids(jax.random.fold_in(key_of[23], 71), 0),
        "group_prob": jnp.clip(0.3 + 0.7 * jax.random.uniform(key_of[18], (SEQUENCE_TOKENS,), jnp.float32) ** block_scale(key_of[18], (SEQUENCE_TOKENS,), ((0, 32),), -0.2, 0.2), 0.3, 1.0),
        "pick_gap": noise(key_of[19], (SEQUENCE_TOKENS,), 1.5, 6.0, ((0, 32),), jnp.float32),
        "w_gate": noise(key_of[20], (EXPERTS, D, FFN_HIDDEN), D ** -0.5, 0.125, ((0, 32),)),
        "w_up": noise(key_of[21], (EXPERTS, D, FFN_HIDDEN), D ** -0.5, 0.125, ((0, 32),)),
        "w_down": noise(key_of[22], (EXPERTS, FFN_HIDDEN, D), (FFN_HIDDEN // 8) ** -0.5, 0.5, ((0, 32),)),
    }


EPSILON = 1e-06
GATE_SCALE = 8.0

def causal_taps(source, weights):
    length = source.shape[0]
    tap_count = weights.shape[0]
    padded = jnp.pad(source.astype(jnp.float32), ((tap_count - 1, 0), (0, 0)))
    total = jnp.zeros(source.shape, jnp.float32)
    for offset in range(tap_count):
        total = total + weights[offset].astype(jnp.float32)[None, :] * padded[offset:offset + length]
    return total.astype(jnp.bfloat16)

def recurrence_inputs(conv_out, rec_gate, inp_gate, decay, jump_log):
    length = conv_out.shape[0]
    head_count = rec_gate.shape[0]
    head_dim = rec_gate.shape[1]
    blocks = conv_out.astype(jnp.float32).reshape(length, head_count, head_dim)
    recur = jax.nn.sigmoid(jnp.einsum('thi,hij->thj', blocks, rec_gate.astype(jnp.float32)).reshape(length, -1))
    admit = jax.nn.sigmoid(jnp.einsum('thi,hij->thj', blocks, inp_gate.astype(jnp.float32)).reshape(length, -1))
    log_decay = -GATE_SCALE * recur * jax.nn.softplus(-decay)[None, :] + jump_log[:, None]
    drive = jnp.sqrt(-jnp.expm1(2.0 * log_decay)) * admit * conv_out.astype(jnp.float32)
    return (jnp.exp(log_decay), drive)

def link_states(earlier, later):
    return (earlier[0] * later[0], later[0] * earlier[1] + later[1])

def block_slots(block_ids):
    onehot = (block_ids[:, None] == jnp.arange(EXPERTS, dtype=jnp.int32)[None, :]).astype(jnp.int32)
    return (lax.optimization_barrier(jnp.sum(jnp.cumsum(onehot, axis=0) * onehot, axis=1)) - 1).astype(jnp.int32)

def route_experts(normed, expert_ids, w_gate, w_up, w_down):
    block_total = SEQUENCE_TOKENS // ROWS
    flat_ids = expert_ids.reshape(block_total, 2 * ROWS).astype(jnp.int32)
    slots = lax.map(block_slots, flat_ids)
    block_index = jnp.broadcast_to(jnp.arange(block_total, dtype=jnp.int32)[:, None], flat_ids.shape)
    token_index = (block_index * ROWS + jnp.arange(2 * ROWS, dtype=jnp.int32)[None, :] // 2).astype(jnp.int32)
    table = jnp.full((EXPERTS, block_total, CAP), SEQUENCE_TOKENS, jnp.int32).at[flat_ids, block_index, slots].set(token_index)
    padded_rows = jnp.concatenate([normed, jnp.zeros((1, D), jnp.bfloat16)], axis=0)

    def one_expert(operands):
        gate_weight, up_weight, down_weight, index_rows = operands
        rows_in = padded_rows[index_rows.reshape(-1)]
        gate_part = jnp.dot(rows_in, gate_weight, preferred_element_type=jnp.float32)
        up_part = jnp.dot(rows_in, up_weight, preferred_element_type=jnp.float32)
        inner = (jax.nn.silu(gate_part) * up_part).astype(jnp.bfloat16)
        return jnp.dot(inner, down_weight, preferred_element_type=jnp.float32).astype(jnp.bfloat16)
    outputs = lax.map(one_expert, (w_gate, w_up, w_down, table))
    place = (flat_ids * (block_total * CAP) + block_index * CAP + slots).reshape(-1).astype(jnp.int32)
    picked = outputs.reshape(-1, D)[place]
    return picked.reshape(SEQUENCE_TOKENS, 2, D)

def reference(stream, conv_in_a, conv_in_b, gate_in_a, gate_in_b, conv_w_a, conv_w_b, rec_gate_a, inp_gate_a, rec_gate_b, inp_gate_b, decay_a, decay_b, decay_increments, out_w_a, out_w_b, norm_gain, expert_ids, group_prob, pick_gap, w_gate, w_up, w_down):
    conv_a = causal_taps(conv_in_a, conv_w_a)
    conv_b = causal_taps(conv_in_b, conv_w_b)
    factor_a, drive_a = recurrence_inputs(conv_a, rec_gate_a, inp_gate_a, decay_a, decay_increments)
    factor_b, drive_b = recurrence_inputs(conv_b, rec_gate_b, inp_gate_b, decay_b, decay_increments)
    states_a = lax.associative_scan(link_states, (factor_a, drive_a), axis=0)[1]
    states_b = lax.associative_scan(link_states, (factor_b, drive_b), axis=0)[1]
    hidden_a = (states_a * jax.nn.gelu(gate_in_a.astype(jnp.float32))).astype(jnp.bfloat16)
    hidden_b = (states_b * jax.nn.gelu(gate_in_b.astype(jnp.float32))).astype(jnp.bfloat16)
    mixed_rows = jnp.dot(hidden_a, out_w_a, preferred_element_type=jnp.float32) + jnp.dot(hidden_b, out_w_b, preferred_element_type=jnp.float32)
    middle = (stream.astype(jnp.float32) + mixed_rows).astype(jnp.bfloat16)
    middle_f = middle.astype(jnp.float32)
    scale_rows = lax.rsqrt(lax.optimization_barrier(jnp.mean(middle_f * middle_f, axis=-1, keepdims=True)) + EPSILON)
    normed = (middle_f * scale_rows * norm_gain.astype(jnp.float32)[None, :]).astype(jnp.bfloat16)
    picked = route_experts(normed, expert_ids, w_gate, w_up, w_down)
    first_weight = group_prob * jax.nn.sigmoid(pick_gap)
    second_weight = group_prob * jax.nn.sigmoid(-pick_gap)
    total = middle_f + first_weight[:, None] * picked[:, 0].astype(jnp.float32) + second_weight[:, None] * picked[:, 1].astype(jnp.float32)
    return total.astype(jnp.bfloat16)
```

```python
import functools

import jax
import jax.numpy as jnp
from jax import lax
from jax.experimental import pallas as pl
from jax.experimental.pallas import tpu as pltpu
from jax.sharding import PartitionSpec as P

EPSILON = 1e-06
GATE_SCALE = 8.0
MESH = pl.DeviceIdType.MESH
VMEM_LIMIT = 60 * 1024 * 1024
RIM = 16


def greet(peers):
    barrier = pltpu.get_barrier_semaphore()
    for device in peers:
        pl.semaphore_signal(barrier, inc=1, device_id=device, device_id_type=MESH)
    pl.semaphore_wait(barrier, len(peers))


def front_kernel(
    sp_count, xa, xb, ga, gb, taps, gates, slope, jumps, hidden,
    padded, conv, gelu_out, factors, states, tail, ends, tail_send, tail_recv, end_send, end_recv,
):
    length, half = xa.shape
    width = 2 * half
    sp, tp = lax.axis_index("sp"), lax.axis_index("tp")

    def peer(k):
        return (lax.rem(sp + k, sp_count), tp)

    greet([peer(k) for k in range(1, sp_count)])
    copies = []
    for i, x in enumerate((xa, xb)):
        copy = pltpu.make_async_remote_copy(
            src_ref=x.at[pl.ds(length - RIM, RIM)], dst_ref=tail.at[i],
            send_sem=tail_send.at[i], recv_sem=tail_recv.at[i],
            device_id=peer(1), device_id_type=MESH,
        )
        copy.start()
        copies.append(copy)
    gelu_out[:, :half] = jax.nn.gelu(ga[...].astype(jnp.float32))
    gelu_out[:, half:] = jax.nn.gelu(gb[...].astype(jnp.float32))
    padded[RIM:, :half] = xa[...].astype(jnp.float32)
    padded[RIM:, half:] = xb[...].astype(jnp.float32)
    for copy in copies:
        copy.wait()
    keep = jnp.where(sp > 0, 1.0, 0.0).astype(jnp.float32)
    padded[:RIM, :half] = tail[0].astype(jnp.float32) * keep
    padded[:RIM, half:] = tail[1].astype(jnp.float32) * keep
    tap_count = taps.shape[0]
    total = jnp.zeros((length, width), jnp.float32)
    for offset in range(tap_count):
        lag = tap_count - 1 - offset
        total = total + taps[offset : offset + 1, :].astype(jnp.float32) * padded[pl.ds(RIM - lag, length), :]
    conv[...] = total.astype(jnp.bfloat16)
    block = gates.shape[1]
    for i in range(gates.shape[0]):
        span = slice(i * block, (i + 1) * block)
        c = conv[:, span]
        both = jnp.dot(c, gates[i], preferred_element_type=jnp.float32)
        recur = jax.nn.sigmoid(both[:, :block])
        admit = jax.nn.sigmoid(both[:, block:])
        log_decay = recur * slope[:, span] + jumps[...]
        factors[:, span] = jnp.exp(log_decay)
        y = 2.0 * log_decay
        series = -y * (1.0 + y * (1 / 2) * (1.0 + y * (1 / 3) * (1.0 + y * (1 / 4) * (1.0 + y * (1 / 5) * (1.0 + y * (1 / 6))))))
        gap = jnp.where(y > -0.25, series, 1.0 - jnp.exp(y))
        states[:, span] = jnp.sqrt(gap) * admit * c.astype(jnp.float32)
    group = 8
    row = lax.broadcasted_iota(jnp.int32, (group, width), 0)

    def link(g, carry):
        carry_factor, carry_state = carry
        at = pl.ds(pl.multiple_of(g * group, group), group)
        f, s = factors[at, :], states[at, :]
        shift = 1
        while shift < group:
            inside = row >= shift
            s = s + f * jnp.where(inside, pltpu.roll(s, shift, 0), 0.0)
            f = f * jnp.where(inside, pltpu.roll(f, shift, 0), 1.0)
            shift *= 2
        s = s + f * carry_state
        f = f * carry_factor
        factors[at, :] = f
        states[at, :] = s
        return f[group - 1 :, :], s[group - 1 :, :]

    one, zero = jnp.ones((1, width), jnp.float32), jnp.zeros((1, width), jnp.float32)
    last_factor, last_state = lax.fori_loop(0, length // group, link, (one, zero), unroll=8)
    ends[sp] = jnp.where(row == 0, last_factor, last_state)
    copies = []
    for k in range(1, sp_count):
        copy = pltpu.make_async_remote_copy(
            src_ref=ends.at[sp], dst_ref=ends.at[sp],
            send_sem=end_send.at[k], recv_sem=end_recv.at[k],
            device_id=peer(k), device_id_type=MESH,
        )
        copy.start()
        copies.append(copy)
    for copy in copies:
        copy.wait()

    def join(position, carried):
        longer = ends[position, 0:1, :] * carried + ends[position, 1:2, :]
        return jnp.where(position < sp, longer, carried)

    carried = lax.fori_loop(0, sp_count, join, zero)
    hidden[...] = ((states[...] + factors[...] * carried) * gelu_out[...]).astype(jnp.bfloat16)


def front(xa, xb, ga, gb, taps, gates, slope, jumps):
    sp_count = lax.axis_size("sp")
    length, half = xa.shape
    width = 2 * half
    vmem = pl.BlockSpec(memory_space=pltpu.VMEM)
    dma = pltpu.SemaphoreType.DMA
    return pl.pallas_call(
        functools.partial(front_kernel, sp_count),
        out_shape=jax.ShapeDtypeStruct((length, width), jnp.bfloat16),
        in_specs=[vmem] * 8,
        out_specs=vmem,
        scratch_shapes=[
            pltpu.VMEM((length + RIM, width), jnp.float32),
            pltpu.VMEM((length, width), jnp.bfloat16),
            pltpu.VMEM((length, width), jnp.float32),
            pltpu.VMEM((length, width), jnp.float32),
            pltpu.VMEM((length, width), jnp.float32),
            pltpu.VMEM((2, RIM, half), jnp.bfloat16),
            pltpu.VMEM((sp_count, 8, width), jnp.float32),
            dma((2,)), dma((2,)), dma((sp_count,)), dma((sp_count,)),
        ],
        compiler_params=pltpu.CompilerParams(
            collective_id=0, has_side_effects=True, vmem_limit_bytes=VMEM_LIMIT
        ),
    )(xa, xb, ga, gb, taps, gates, slope, jumps)


def mix_kernel(
    cuts, hidden, wa, wb, stream, gain, middle, normed,
    out_pair, in_pair, own, out_far, in_far, pair_send, pair_recv, far_send, far_recv,
):
    sp, tp = lax.axis_index("sp"), lax.axis_index("tp")
    rows = stream.shape[0]
    half = wa.shape[0]
    x, core = tp // 2, lax.rem(tp, 2)
    partner, across = (sp, x * 2 + 1 - core), (sp, (1 - x) * 2 + core)
    greet([partner, across])

    def part(owner):
        h = hidden[pl.ds(pl.multiple_of(owner * rows, rows), rows), :]
        return jnp.dot(h[:, :half], wa[...], preferred_element_type=jnp.float32) + jnp.dot(
            h[:, half:], wb[...], preferred_element_type=jnp.float32
        )

    pair = []
    for i, chip in enumerate((1 - x, x)):
        out_pair[i] = part(chip * 2 + 1 - core).astype(jnp.bfloat16)
        copy = pltpu.make_async_remote_copy(
            src_ref=out_pair.at[i], dst_ref=in_pair.at[i],
            send_sem=pair_send.at[i], recv_sem=pair_recv.at[i],
            device_id=partner, device_id_type=MESH,
        )
        copy.start()
        pair.append(copy)
    own[...] = part((1 - x) * 2 + core)
    pair[0].wait()
    step = rows // cuts
    far = []
    for j in range(cuts):
        span = pl.ds(j * step, step)
        out_far[span, :] = (own[span, :] + in_pair[0, span, :].astype(jnp.float32)).astype(jnp.bfloat16)
        copy = pltpu.make_async_remote_copy(
            src_ref=out_far.at[span], dst_ref=in_far.at[span],
            send_sem=far_send.at[j], recv_sem=far_recv.at[j],
            device_id=across, device_id_type=MESH,
        )
        copy.start()
        far.append(copy)
    own[...] = part(x * 2 + core)
    pair[1].wait()
    own[...] = own[...] + in_pair[1].astype(jnp.float32) + stream[...].astype(jnp.float32)
    for j in range(cuts):
        span = pl.ds(j * step, step)
        far[j].wait()
        m = (own[span, :] + in_far[span, :].astype(jnp.float32)).astype(jnp.bfloat16)
        middle[span, :] = m
        mf = m.astype(jnp.float32)
        scale = lax.rsqrt(jnp.mean(mf * mf, axis=-1, keepdims=True) + EPSILON)
        normed[span, :] = (mf * scale * gain[...].astype(jnp.float32)).astype(jnp.bfloat16)


def mix(hidden, wa, wb, stream, gain):
    rows, width = stream.shape
    cuts = 4
    vmem = pl.BlockSpec(memory_space=pltpu.VMEM)
    dma = pltpu.SemaphoreType.DMA
    shape = jax.ShapeDtypeStruct((rows, width), jnp.bfloat16)
    return pl.pallas_call(
        functools.partial(mix_kernel, cuts),
        out_shape=(shape, shape),
        in_specs=[vmem] * 5,
        out_specs=(vmem, vmem),
        scratch_shapes=[
            pltpu.VMEM((2, rows, width), jnp.bfloat16),
            pltpu.VMEM((2, rows, width), jnp.bfloat16),
            pltpu.VMEM((rows, width), jnp.float32),
            pltpu.VMEM((rows, width), jnp.bfloat16),
            pltpu.VMEM((rows, width), jnp.bfloat16),
            dma((2,)), dma((2,)), dma((cuts,)), dma((cuts,)),
        ],
        compiler_params=pltpu.CompilerParams(
            collective_id=1, has_side_effects=True, vmem_limit_bytes=VMEM_LIMIT
        ),
    )(hidden, wa, wb, stream, gain)


def pair_blocks(gate, block):
    heads, dim = gate.shape[0], gate.shape[1]
    join = block // dim
    if join == 1:
        return gate
    pieces = gate.reshape(heads // join, join, dim, dim)
    rows = [
        jnp.pad(pieces[:, i], ((0, 0), (0, 0), (i * dim, (join - 1 - i) * dim))) for i in range(join)
    ]
    return jnp.concatenate(rows, axis=1)


def shards(
    stream,
    conv_in_a,
    conv_in_b,
    gate_in_a,
    gate_in_b,
    conv_w_a,
    conv_w_b,
    rec_gate_a,
    inp_gate_a,
    rec_gate_b,
    inp_gate_b,
    decay_a,
    decay_b,
    decay_increments,
    out_w_a,
    out_w_b,
    norm_gain,
    expert_ids,
    group_prob,
    pick_gap,
    w_gate,
    w_up,
    w_down,
):
    block = max(rec_gate_a.shape[1], rec_gate_b.shape[1])
    recur = jnp.concatenate([pair_blocks(rec_gate_a, block), rec_gate_b], axis=0)
    admit = jnp.concatenate([pair_blocks(inp_gate_a, block), inp_gate_b], axis=0)
    gates = jnp.concatenate([recur, admit], axis=2)
    taps = jnp.concatenate([conv_w_a, conv_w_b], axis=1)
    slope = -GATE_SCALE * jax.nn.softplus(-jnp.concatenate([decay_a, decay_b]))[None, :]
    hidden = front(
        conv_in_a, conv_in_b, gate_in_a, gate_in_b, taps, gates, slope, decay_increments[:, None]
    )
    tp_count = lax.axis_size("tp")
    row_count = stream.shape[0]
    middle, normed = mix(hidden, out_w_a, out_w_b, stream, norm_gain[None, :])
    middle_f = middle.astype(jnp.float32)
    width = normed.shape[1]
    sequence_parallel_count = lax.axis_size("sp")
    experts = sequence_parallel_count * tp_count * w_gate.shape[0]
    slot_count = 4 * row_count // experts
    flat_ids = expert_ids.reshape(-1)
    onehot = (flat_ids[:, None] == jnp.arange(experts, dtype=jnp.int32)[None, :]).astype(jnp.int32)
    ranks = jnp.sum(jnp.cumsum(onehot, axis=0) * onehot, axis=1) - 1
    destination = flat_ids * slot_count + ranks
    copies = jnp.repeat(normed, expert_ids.shape[1], axis=0)
    buffer = jnp.zeros((experts * slot_count, width), jnp.bfloat16).at[destination].set(copies)
    buffer = buffer.reshape(experts, slot_count, width)
    arrived = lax.all_to_all(buffer, ("sp", "tp"), split_axis=0, concat_axis=0, tiled=True)
    flat_rows = arrived.reshape(-1, arrived.shape[-1])
    gate_part = jnp.dot(flat_rows, w_gate[0], preferred_element_type=jnp.float32)
    up_part = jnp.dot(flat_rows, w_up[0], preferred_element_type=jnp.float32)
    inner = (jax.nn.silu(gate_part) * up_part).astype(jnp.bfloat16)
    served = jnp.dot(inner, w_down[0], preferred_element_type=jnp.float32).astype(jnp.bfloat16)
    returned = lax.all_to_all(
        served.reshape(arrived.shape), ("sp", "tp"), split_axis=0, concat_axis=0, tiled=True
    )
    returned = returned.reshape(experts * slot_count, width)
    picked = returned[destination].reshape(row_count, expert_ids.shape[1], width)
    first_weight = group_prob * jax.nn.sigmoid(pick_gap)
    second_weight = group_prob * jax.nn.sigmoid(-pick_gap)
    total = (
        middle_f
        + first_weight[:, None] * picked[:, 0].astype(jnp.float32)
        + second_weight[:, None] * picked[:, 1].astype(jnp.float32)
    )
    return total.astype(jnp.bfloat16)


def solution(mesh):
    placed = (
        P(("sp", "tp"), None),
        P("sp", "tp"),
        P("sp", "tp"),
        P("sp", "tp"),
        P("sp", "tp"),
        P(None, "tp"),
        P(None, "tp"),
        P("tp", None, None),
        P("tp", None, None),
        P("tp", None, None),
        P("tp", None, None),
        P("tp"),
        P("tp"),
        P("sp"),
        P("tp", None),
        P("tp", None),
        P(),
        P(("sp", "tp"), None),
        P(("sp", "tp")),
        P(("sp", "tp")),
        P(("sp", "tp"), None, None),
        P(("sp", "tp"), None, None),
        P(("sp", "tp"), None, None),
    )
    return jax.shard_map(
        shards, mesh=mesh, in_specs=placed, out_specs=P(("sp", "tp"), None), check_vma=False
    )
```

```python
import functools

import jax
import jax.numpy as jnp
from jax import lax
from jax.experimental import pallas as pl
from jax.experimental.pallas import tpu as pltpu
from jax.sharding import PartitionSpec as P

EPSILON = 1e-06
GATE_SCALE = 8.0
GROUPS = 4
MESH = pl.DeviceIdType.MESH
VMEM_LIMIT = 60 * 1024 * 1024
RIM = 16


def greet(peers):
    barrier = pltpu.get_barrier_semaphore()
    for device in peers:
        pl.semaphore_signal(barrier, inc=1, device_id=device, device_id_type=MESH)
    pl.semaphore_wait(barrier, len(peers))


def front_kernel(
    sp_count, xa, xb, ga, gb, taps, gates, slope, jumps, hidden,
    padded, conv, gelu_out, factors, states, tail, ends, tail_send, tail_recv, end_send, end_recv,
):
    length, half = xa.shape
    width = 2 * half
    sp, tp = lax.axis_index("sp"), lax.axis_index("tp")

    def peer(k):
        return (lax.rem(sp + k, sp_count), tp)

    greet([peer(k) for k in range(1, sp_count)])
    copies = []
    for i, x in enumerate((xa, xb)):
        copy = pltpu.make_async_remote_copy(
            src_ref=x.at[pl.ds(length - RIM, RIM)], dst_ref=tail.at[i],
            send_sem=tail_send.at[i], recv_sem=tail_recv.at[i],
            device_id=peer(1), device_id_type=MESH,
        )
        copy.start()
        copies.append(copy)
    gelu_out[:, :half] = jax.nn.gelu(ga[...].astype(jnp.float32))
    gelu_out[:, half:] = jax.nn.gelu(gb[...].astype(jnp.float32))
    padded[RIM:, :half] = xa[...].astype(jnp.float32)
    padded[RIM:, half:] = xb[...].astype(jnp.float32)
    for copy in copies:
        copy.wait()
    keep = jnp.where(sp > 0, 1.0, 0.0).astype(jnp.float32)
    padded[:RIM, :half] = tail[0].astype(jnp.float32) * keep
    padded[:RIM, half:] = tail[1].astype(jnp.float32) * keep
    tap_count = taps.shape[0]
    total = jnp.zeros((length, width), jnp.float32)
    for offset in range(tap_count):
        lag = tap_count - 1 - offset
        total = total + taps[offset : offset + 1, :].astype(jnp.float32) * padded[pl.ds(RIM - lag, length), :]
    conv[...] = total.astype(jnp.bfloat16)
    block = gates.shape[1]
    for i in range(gates.shape[0]):
        span = slice(i * block, (i + 1) * block)
        c = conv[:, span]
        both = jnp.dot(c, gates[i], preferred_element_type=jnp.float32)
        recur = jax.nn.sigmoid(both[:, :block])
        admit = jax.nn.sigmoid(both[:, block:])
        log_decay = recur * slope[:, span] + jumps[...]
        factors[:, span] = jnp.exp(log_decay)
        y = 2.0 * log_decay
        series = -y * (1.0 + y * (1 / 2) * (1.0 + y * (1 / 3) * (1.0 + y * (1 / 4) * (1.0 + y * (1 / 5) * (1.0 + y * (1 / 6))))))
        gap = jnp.where(y > -0.25, series, 1.0 - jnp.exp(y))
        states[:, span] = jnp.sqrt(gap) * admit * c.astype(jnp.float32)
    group = 8
    row = lax.broadcasted_iota(jnp.int32, (group, width), 0)

    def link(g, carry):
        carry_factor, carry_state = carry
        at = pl.ds(pl.multiple_of(g * group, group), group)
        f, s = factors[at, :], states[at, :]
        shift = 1
        while shift < group:
            inside = row >= shift
            s = s + f * jnp.where(inside, pltpu.roll(s, shift, 0), 0.0)
            f = f * jnp.where(inside, pltpu.roll(f, shift, 0), 1.0)
            shift *= 2
        s = s + f * carry_state
        f = f * carry_factor
        factors[at, :] = f
        states[at, :] = s
        return f[group - 1 :, :], s[group - 1 :, :]

    one, zero = jnp.ones((1, width), jnp.float32), jnp.zeros((1, width), jnp.float32)
    last_factor, last_state = lax.fori_loop(0, length // group, link, (one, zero), unroll=8)
    ends[sp] = jnp.where(row == 0, last_factor, last_state)
    copies = []
    for k in range(1, sp_count):
        copy = pltpu.make_async_remote_copy(
            src_ref=ends.at[sp], dst_ref=ends.at[sp],
            send_sem=end_send.at[k], recv_sem=end_recv.at[k],
            device_id=peer(k), device_id_type=MESH,
        )
        copy.start()
        copies.append(copy)
    for copy in copies:
        copy.wait()

    def join(position, carried):
        longer = ends[position, 0:1, :] * carried + ends[position, 1:2, :]
        return jnp.where(position < sp, longer, carried)

    carried = lax.fori_loop(0, sp_count, join, zero)
    hidden[...] = ((states[...] + factors[...] * carried) * gelu_out[...]).astype(jnp.bfloat16)


def front(xa, xb, ga, gb, taps, gates, slope, jumps):
    sp_count = lax.axis_size("sp")
    length, half = xa.shape
    width = 2 * half
    vmem = pl.BlockSpec(memory_space=pltpu.VMEM)
    dma = pltpu.SemaphoreType.DMA
    return pl.pallas_call(
        functools.partial(front_kernel, sp_count),
        out_shape=jax.ShapeDtypeStruct((length, width), jnp.bfloat16),
        in_specs=[vmem] * 8,
        out_specs=vmem,
        scratch_shapes=[
            pltpu.VMEM((length + RIM, width), jnp.float32),
            pltpu.VMEM((length, width), jnp.bfloat16),
            pltpu.VMEM((length, width), jnp.float32),
            pltpu.VMEM((length, width), jnp.float32),
            pltpu.VMEM((length, width), jnp.float32),
            pltpu.VMEM((2, RIM, half), jnp.bfloat16),
            pltpu.VMEM((sp_count, 8, width), jnp.float32),
            dma((2,)), dma((2,)), dma((sp_count,)), dma((sp_count,)),
        ],
        compiler_params=pltpu.CompilerParams(
            collective_id=0, has_side_effects=True, vmem_limit_bytes=VMEM_LIMIT
        ),
    )(xa, xb, ga, gb, taps, gates, slope, jumps)


def mix_kernel(
    cuts, hidden, wa, wb, stream, gain, middle, normed,
    out_pair, in_pair, own, out_far, in_far, pair_send, pair_recv, far_send, far_recv,
):
    sp, tp = lax.axis_index("sp"), lax.axis_index("tp")
    rows = stream.shape[0]
    half = wa.shape[0]
    x, core = tp // 2, lax.rem(tp, 2)
    partner, across = (sp, x * 2 + 1 - core), (sp, (1 - x) * 2 + core)
    greet([partner, across])

    def part(owner):
        h = hidden[pl.ds(pl.multiple_of(owner * rows, rows), rows), :]
        return jnp.dot(h[:, :half], wa[...], preferred_element_type=jnp.float32) + jnp.dot(
            h[:, half:], wb[...], preferred_element_type=jnp.float32
        )

    pair = []
    for i, chip in enumerate((1 - x, x)):
        out_pair[i] = part(chip * 2 + 1 - core).astype(jnp.bfloat16)
        copy = pltpu.make_async_remote_copy(
            src_ref=out_pair.at[i], dst_ref=in_pair.at[i],
            send_sem=pair_send.at[i], recv_sem=pair_recv.at[i],
            device_id=partner, device_id_type=MESH,
        )
        copy.start()
        pair.append(copy)
    own[...] = part((1 - x) * 2 + core)
    pair[0].wait()
    step = rows // cuts
    far = []
    for j in range(cuts):
        span = pl.ds(j * step, step)
        out_far[span, :] = (own[span, :] + in_pair[0, span, :].astype(jnp.float32)).astype(jnp.bfloat16)
        copy = pltpu.make_async_remote_copy(
            src_ref=out_far.at[span], dst_ref=in_far.at[span],
            send_sem=far_send.at[j], recv_sem=far_recv.at[j],
            device_id=across, device_id_type=MESH,
        )
        copy.start()
        far.append(copy)
    own[...] = part(x * 2 + core)
    pair[1].wait()
    own[...] = own[...] + in_pair[1].astype(jnp.float32) + stream[...].astype(jnp.float32)
    for j in range(cuts):
        span = pl.ds(j * step, step)
        far[j].wait()
        m = (own[span, :] + in_far[span, :].astype(jnp.float32)).astype(jnp.bfloat16)
        middle[span, :] = m
        mf = m.astype(jnp.float32)
        scale = lax.rsqrt(jnp.mean(mf * mf, axis=-1, keepdims=True) + EPSILON)
        normed[span, :] = (mf * scale * gain[...].astype(jnp.float32)).astype(jnp.bfloat16)


def mix(hidden, wa, wb, stream, gain):
    rows, width = stream.shape
    cuts = 4
    vmem = pl.BlockSpec(memory_space=pltpu.VMEM)
    dma = pltpu.SemaphoreType.DMA
    shape = jax.ShapeDtypeStruct((rows, width), jnp.bfloat16)
    return pl.pallas_call(
        functools.partial(mix_kernel, cuts),
        out_shape=(shape, shape),
        in_specs=[vmem] * 5,
        out_specs=(vmem, vmem),
        scratch_shapes=[
            pltpu.VMEM((2, rows, width), jnp.bfloat16),
            pltpu.VMEM((2, rows, width), jnp.bfloat16),
            pltpu.VMEM((rows, width), jnp.float32),
            pltpu.VMEM((rows, width), jnp.bfloat16),
            pltpu.VMEM((rows, width), jnp.bfloat16),
            dma((2,)), dma((2,)), dma((cuts,)), dma((cuts,)),
        ],
        compiler_params=pltpu.CompilerParams(
            collective_id=1, has_side_effects=True, vmem_limit_bytes=VMEM_LIMIT
        ),
    )(hidden, wa, wb, stream, gain)


def seat(groups, size, tp_count):
    me = lax.axis_index("sp") * tp_count + lax.axis_index("tp")
    group, member = me // size, lax.rem(me, size)

    def device(g, m):
        flat = lax.rem(g, groups) * size + lax.rem(m, size)
        return (flat // tp_count, lax.rem(flat, tp_count))

    peers = [device(group, member + j) for j in range(1, size)]
    peers += [device(group + k, member) for k in range(1, groups)]
    return group, member, device, peers


def near_first(groups):
    return sorted(range(groups), key=lambda k: (min(k, groups - k), k))


def spread_kernel(
    tp_count, normed, place, meta, arrived, got_meta,
    block, got, pieces, row_send, row_recv, meta_send, meta_recv, piece_send, piece_recv,
):
    groups, size, cap, width = arrived.shape
    slots = place.shape[1]
    group, member, device, peers = seat(groups, size, tp_count)
    greet(peers)
    order = near_first(groups)

    def meta_copy(k):
        return pltpu.make_async_remote_copy(
            src_ref=meta.at[lax.rem(group + k, groups)], dst_ref=got_meta.at[group],
            send_sem=meta_send.at[k], recv_sem=meta_recv.at[k],
            device_id=device(group + k, member), device_id_type=MESH,
        )

    def row_copy(k):
        return pltpu.make_async_remote_copy(
            src_ref=block.at[lax.rem(group + k, groups)], dst_ref=got.at[group],
            send_sem=row_send.at[k], recv_sem=row_recv.at[k],
            device_id=device(group + k, member), device_id_type=MESH,
        )

    def piece_copy(k, j, to, origin):
        source = lax.rem(group - k + groups, groups)
        return pltpu.make_async_remote_copy(
            src_ref=pieces.at[source, to], dst_ref=arrived.at[source, origin],
            send_sem=piece_send.at[k, j], recv_sem=piece_recv.at[k, j],
            device_id=device(group, to), device_id_type=MESH,
        )

    for k in order[1:]:
        meta_copy(k).start()
    for k in order[1:]:
        to = lax.rem(group + k, groups)
        block[to] = jnp.dot(place[to], normed[...], preferred_element_type=jnp.float32).astype(jnp.bfloat16)
        row_copy(k).start()
    got[group] = jnp.dot(place[group], normed[...], preferred_element_type=jnp.float32).astype(jnp.bfloat16)
    got_meta[group] = meta[group]
    slot = lax.broadcasted_iota(jnp.int32, (size * cap, slots), 0).astype(jnp.float32)
    for k in order:
        source = lax.rem(group - k + groups, groups)
        if k:
            meta_copy(k).wait_recv()
            row_copy(k).wait_recv()
        info = got_meta[source]
        pick = jnp.where((slot == info[0:1, :slots]) | (slot == info[1:2, :slots]), 1.0, 0.0)
        rows = jnp.dot(pick.astype(jnp.bfloat16), got[source], preferred_element_type=jnp.float32)
        for e in range(size):
            pieces[source, e] = rows[e * cap : (e + 1) * cap].astype(jnp.bfloat16)

        def send(j, carry, k=k):
            piece_copy(k, j, lax.rem(member + j, size), member).start()
            return carry

        lax.fori_loop(1, size, send, 0)
        arrived[source, member] = pieces[source, member]
    for k in order[1:]:
        meta_copy(k).wait_send()
        row_copy(k).wait_send()
    for k in order:

        def finish(j, carry, k=k):
            piece_copy(k, j, lax.rem(member + j, size), lax.rem(member - j + size, size)).wait()
            return carry

        lax.fori_loop(1, size, finish, 0)


def spread(normed, place, meta, size, cap):
    groups, slots, _ = place.shape
    width = normed.shape[1]
    vmem = pl.BlockSpec(memory_space=pltpu.VMEM)
    dma = pltpu.SemaphoreType.DMA
    return pl.pallas_call(
        functools.partial(spread_kernel, lax.axis_size("tp")),
        out_shape=(
            jax.ShapeDtypeStruct((groups, size, cap, width), jnp.bfloat16),
            jax.ShapeDtypeStruct(meta.shape, meta.dtype),
        ),
        in_specs=[vmem] * 3,
        out_specs=(vmem, vmem),
        scratch_shapes=[
            pltpu.VMEM((groups, slots, width), jnp.bfloat16),
            pltpu.VMEM((groups, slots, width), jnp.bfloat16),
            pltpu.VMEM((groups, size, cap, width), jnp.bfloat16),
            dma((groups,)), dma((groups,)), dma((groups,)), dma((groups,)),
            dma((groups, size)), dma((groups, size)),
        ],
        compiler_params=pltpu.CompilerParams(
            collective_id=2, has_side_effects=True, vmem_limit_bytes=VMEM_LIMIT
        ),
    )(normed, place, meta)


def collect_kernel(
    tp_count, served, got_meta, middle, put, out,
    held, outgoing, back, total, piece_send, piece_recv, row_send, row_recv,
):
    groups, size, cap, width = served.shape
    slots = put.shape[2]
    group, member, device, peers = seat(groups, size, tp_count)
    greet(peers)
    order = near_first(groups)[::-1]

    def piece_copy(k, j, to, origin):
        source = lax.rem(group - k + groups, groups)
        return pltpu.make_async_remote_copy(
            src_ref=served.at[source, to], dst_ref=held.at[source, origin],
            send_sem=piece_send.at[k, j], recv_sem=piece_recv.at[k, j],
            device_id=device(group, to), device_id_type=MESH,
        )

    def row_copy(k, origin):
        return pltpu.make_async_remote_copy(
            src_ref=outgoing.at[k], dst_ref=back.at[origin],
            send_sem=row_send.at[k], recv_sem=row_recv.at[k],
            device_id=device(group - k + groups, member), device_id_type=MESH,
        )

    for k in order:

        def send(j, carry, k=k):
            piece_copy(k, j, lax.rem(member + j, size), member).start()
            return carry

        lax.fori_loop(1, size, send, 0)
    lane = lax.broadcasted_iota(jnp.int32, (slots, size * cap), 1).astype(jnp.float32)
    total[...] = middle[...].astype(jnp.float32)
    for k in order:
        source = lax.rem(group - k + groups, groups)
        held[source, member] = served[source, member]

        def finish(j, carry, k=k):
            piece_copy(k, j, lax.rem(member + j, size), lax.rem(member - j + size, size)).wait()
            return carry

        lax.fori_loop(1, size, finish, 0)
        if cap % 16:
            rows = jnp.concatenate(
                [held[source, e].astype(jnp.float32) for e in range(size)], axis=0
            ).astype(jnp.bfloat16)
        else:
            rows = held[source].reshape(size * cap, width)
        info = got_meta[source].T[:slots]
        first = jnp.dot(
            jnp.where(info[:, 0:1] == lane, 1.0, 0.0).astype(jnp.bfloat16), rows,
            preferred_element_type=jnp.float32,
        )
        second = jnp.dot(
            jnp.where(info[:, 1:2] == lane, 1.0, 0.0).astype(jnp.bfloat16), rows,
            preferred_element_type=jnp.float32,
        )
        joined = (info[:, 2:3] * first + info[:, 3:4] * second).astype(jnp.bfloat16)
        if k:
            outgoing[k] = joined
            row_copy(k, group).start()
        else:
            total[...] += jnp.dot(put[group], joined, preferred_element_type=jnp.float32)
    for k in order:
        if k:
            origin = lax.rem(group + k, groups)
            row_copy(k, origin).wait()
            total[...] += jnp.dot(put[origin], back[origin], preferred_element_type=jnp.float32)
    out[...] = total[...].astype(jnp.bfloat16)


def collect(served, got_meta, middle, put):
    groups, size, cap, width = served.shape
    slots = put.shape[2]
    vmem = pl.BlockSpec(memory_space=pltpu.VMEM)
    dma = pltpu.SemaphoreType.DMA
    return pl.pallas_call(
        functools.partial(collect_kernel, lax.axis_size("tp")),
        out_shape=jax.ShapeDtypeStruct(middle.shape, jnp.bfloat16),
        in_specs=[vmem] * 4,
        out_specs=vmem,
        scratch_shapes=[
            pltpu.VMEM((groups, size, cap, width), jnp.bfloat16),
            pltpu.VMEM((groups, slots, width), jnp.bfloat16),
            pltpu.VMEM((groups, slots, width), jnp.bfloat16),
            pltpu.VMEM(middle.shape, jnp.float32),
            dma((groups, size)), dma((groups, size)), dma((groups,)), dma((groups,)),
        ],
        compiler_params=pltpu.CompilerParams(
            collective_id=3, has_side_effects=True, vmem_limit_bytes=VMEM_LIMIT
        ),
    )(served, got_meta, middle, put)


def routes(expert_ids, group_prob, pick_gap, experts, cap):
    row_count = expert_ids.shape[0]
    size = experts // GROUPS
    slots = size * cap // 2
    flat_ids = expert_ids.reshape(-1)
    onehot = (flat_ids[:, None] == jnp.arange(experts, dtype=jnp.int32)[None, :]).astype(jnp.int32)
    ranks = (jnp.sum(jnp.cumsum(onehot, axis=0) * onehot, axis=1) - 1).reshape(row_count, -1)
    positions = ((expert_ids % size) * cap + ranks + 1).astype(jnp.float32)
    group = expert_ids[:, 0] // size
    mine = (group[:, None] == jnp.arange(GROUPS, dtype=jnp.int32)[None, :]).astype(jnp.int32)
    slot = group * slots + jnp.sum(jnp.cumsum(mine, axis=0) * mine, axis=1) - 1
    index = jnp.arange(GROUPS * slots, dtype=jnp.int32)
    hit = index[:, None] == slot[None, :]
    place = hit.astype(jnp.bfloat16).reshape(GROUPS, slots, row_count)
    values = jnp.stack([
        positions[:, 0],
        positions[:, 1],
        group_prob * jax.nn.sigmoid(pick_gap),
        group_prob * jax.nn.sigmoid(-pick_gap),
    ])
    spots = jnp.sum(jnp.where(hit[None], values[:, None, :], 0.0), axis=2)
    spots = spots - jnp.array([1.0, 1.0, 0.0, 0.0], jnp.float32)[:, None]
    spots = jnp.transpose(spots.reshape(4, GROUPS, slots), (1, 0, 2))
    lanes = -(-slots // 128) * 128
    meta = jnp.pad(spots, ((0, 0), (0, 4), (0, lanes - slots)))
    return place, jnp.transpose(place, (0, 2, 1)), meta


def pair_blocks(gate, block):
    heads, dim = gate.shape[0], gate.shape[1]
    join = block // dim
    if join == 1:
        return gate
    pieces = gate.reshape(heads // join, join, dim, dim)
    rows = [
        jnp.pad(pieces[:, i], ((0, 0), (0, 0), (i * dim, (join - 1 - i) * dim))) for i in range(join)
    ]
    return jnp.concatenate(rows, axis=1)


def shards(
    stream,
    conv_in_a,
    conv_in_b,
    gate_in_a,
    gate_in_b,
    conv_w_a,
    conv_w_b,
    rec_gate_a,
    inp_gate_a,
    rec_gate_b,
    inp_gate_b,
    decay_a,
    decay_b,
    decay_increments,
    out_w_a,
    out_w_b,
    norm_gain,
    expert_ids,
    group_prob,
    pick_gap,
    w_gate,
    w_up,
    w_down,
):
    block = max(rec_gate_a.shape[1], rec_gate_b.shape[1])
    recur = jnp.concatenate([pair_blocks(rec_gate_a, block), rec_gate_b], axis=0)
    admit = jnp.concatenate([pair_blocks(inp_gate_a, block), inp_gate_b], axis=0)
    gates = jnp.concatenate([recur, admit], axis=2)
    taps = jnp.concatenate([conv_w_a, conv_w_b], axis=1)
    slope = -GATE_SCALE * jax.nn.softplus(-jnp.concatenate([decay_a, decay_b]))[None, :]
    hidden = front(
        conv_in_a, conv_in_b, gate_in_a, gate_in_b, taps, gates, slope, decay_increments[:, None]
    )
    tp_count = lax.axis_size("tp")
    row_count = stream.shape[0]
    middle, normed = mix(hidden, out_w_a, out_w_b, stream, norm_gain[None, :])
    experts = lax.axis_size("sp") * tp_count * w_gate.shape[0]
    cap = 4 * row_count // experts
    place, put, meta = routes(expert_ids, group_prob, pick_gap, experts, cap)
    arrived, got_meta = spread(normed, place, meta, experts // GROUPS, cap)
    flat_rows = arrived.reshape(-1, arrived.shape[-1])
    gate_part = jnp.dot(flat_rows, w_gate[0], preferred_element_type=jnp.float32)
    up_part = jnp.dot(flat_rows, w_up[0], preferred_element_type=jnp.float32)
    inner = (jax.nn.silu(gate_part) * up_part).astype(jnp.bfloat16)
    served = jnp.dot(inner, w_down[0], preferred_element_type=jnp.float32).astype(jnp.bfloat16)
    return collect(served.reshape(arrived.shape), got_meta, middle, put)


def solution(mesh):
    placed = (
        P(("sp", "tp"), None),
        P("sp", "tp"),
        P("sp", "tp"),
        P("sp", "tp"),
        P("sp", "tp"),
        P(None, "tp"),
        P(None, "tp"),
        P("tp", None, None),
        P("tp", None, None),
        P("tp", None, None),
        P("tp", None, None),
        P("tp"),
        P("tp"),
        P("sp"),
        P("tp", None),
        P("tp", None),
        P(),
        P(("sp", "tp"), None),
        P(("sp", "tp")),
        P(("sp", "tp")),
        P(("sp", "tp"), None, None),
        P(("sp", "tp"), None, None),
        P(("sp", "tp"), None, None),
    )
    return jax.shard_map(
        shards, mesh=mesh, in_specs=placed, out_specs=P(("sp", "tp"), None), check_vma=False
    )
```
